32 devices in a mesh: fs: 8 (over z, x), tp: 4 (over y, core).
Axes of the slice: x: 2, y: 2, z: 4, core: 2. Of those that a mesh axis runs over, the one named last changes fastest.
Arguments:
- normed_inputs: bfloat16 [24576, 2048], P(('fs', 'tp')), may hold values from -6 to 6
- query_cotangent: bfloat16 [24576, 1024], P(('fs', 'tp')), may hold values from -6 to 6
- head_outputs: bfloat16 [24576, 1024], P(('fs', 'tp')), may hold values from -6 to 6
- output_cotangent: bfloat16 [24576, 2048], P(('fs', 'tp')), may hold values from -6 to 6
- query_weight: float32 [2048, 1024], P('fs', 'tp'), may hold values from -0.125 to 0.125
- out_weight: float32 [1024, 2048], P('fs', 'tp'), may hold values from -0.1875 to 0.1875
- query_basis: bfloat16 [2048, 512], P('fs'), may hold values from -0.125 to 0.125
- out_basis: bfloat16 [1024, 512], P('fs'), may hold values from -0.1875 to 0.1875
- query_mean: float32 [512, 1024], P('fs', 'tp'), may hold values from -6 to 6
- query_square: float32 [512, 1024], P('fs', 'tp'), may hold values from 0.5 to 2
- out_mean: float32 [512, 2048], P('fs', 'tp'), may hold values from -6 to 6
- out_square: float32 [512, 2048], P('fs', 'tp'), may hold values from 0.5 to 2
Outputs:
- query_mean_new: float32 [512, 1024], P('fs', 'tp')
- query_square_new: float32 [512, 1024], P('fs', 'tp')
- query_step: float32 [2048, 1024], P('fs', 'tp')
- query_weight_new: float32 [2048, 1024], P('fs', 'tp')
- query_copy: bfloat16 [2048, 1024], P(None, 'tp')
- out_mean_new: float32 [512, 2048], P('fs', 'tp')
- out_square_new: float32 [512, 2048], P('fs', 'tp')
- out_step: float32 [1024, 2048], P('fs', 'tp')
- out_weight_new: float32 [1024, 2048], P('fs', 'tp')
- out_copy: bfloat16 [1024, 2048], P(None, 'tp')
The draws below stay inside these ranges and needn't reach their ends.
All inputs are finite; a program needn't handle non-finite values.
Results may differ from the reference program's by a relative error of at most 0.009.
Values may be sent and summed in bfloat16 or wider, within the bound.
A program may use at most 64 MiB of HBM per device.

```python
import math
import jax
import jax.numpy as jnp
from jax import lax

D = 2048
QW = 1024
RANK = 512
TOK_DEV = 768
TOKENS = 24576


def strengthened(array, stream_key, source, target, blocks, factor):
    def block_of(position):
        return (jnp.arange(array.shape[position]) // (array.shape[position] // blocks)).reshape((-1,) + (1,) * (array.ndim - 1 - position))

    one_side = jax.random.permutation(stream_key, blocks)[block_of(target)]
    second = (block_of(target) + blocks // 2) % blocks
    return jnp.where((block_of(source) == one_side) | (block_of(source) == second), factor * array, array)


def block_scale(own_key, extent, shards, least, top_value):
    loudness, own = 1.0, jax.random.fold_in(own_key, 6)
    for axis_at, shards_of in shards:
        heights = jnp.exp(jax.random.uniform(jax.random.fold_in(own, axis_at), (shards_of,), jnp.float32, least / len(shards), top_value / len(shards)))
        loudness = loudness * jnp.repeat(heights, extent[axis_at] // shards_of).reshape([-1 if axis == axis_at else 1 for axis in range(len(extent))])
    return loudness


def normal_values(own_key, extent, deviation, reach, cuts=(), kind=jnp.bfloat16):
    loudness = block_scale(own_key, extent, cuts, -0.22, 0.18) if cuts else 1.0
    result = jax.random.normal(own_key, extent, jnp.float32) * deviation * loudness
    return jnp.minimum(jnp.maximum(result, -reach), reach).astype(kind)


def heavy_noise(stream_key, dims, scale, limit, shards, heavy, dtype=jnp.bfloat16):
    result = scale * jax.random.normal(stream_key, dims, jnp.float32)
    if shards:
        result = result * block_scale(stream_key, dims, shards, -0.22, 0.18)
    return jnp.clip(strengthened(result, jax.random.fold_in(stream_key, 3), *heavy), -limit, limit).astype(dtype)


def setup_inputs(seed: int = 0) -> dict:
    seeds = jax.random.split(jax.random.key(seed), 13)
    normed_inputs = heavy_noise(seeds[0], (TOKENS, D), 1.0, 6.0, ((0, 32),), (0, 1, 32, 2.75))
    query_cotangent = normal_values(seeds[1], (TOKENS, QW), 1.0, 6.0, ((0, 32),))
    head_outputs = heavy_noise(seeds[2], (TOKENS, QW), 1.0, 6.0, ((0, 32),), (0, 1, 32, 2.75))
    output_cotangent = normal_values(seeds[3], (TOKENS, D), 1.0, 6.0, ((0, 32),))
    query_weight = normal_values(seeds[4], (D, QW), D ** -0.5, 0.125, ((0, 8), (1, 4)), jnp.float32)
    out_weight = normal_values(seeds[5], (QW, D), QW ** -0.5, 0.1875, ((0, 8), (1, 4)), jnp.float32)
    query_basis = normal_values(seeds[6], (D, RANK), D ** -0.5, 0.125, ((0, 8),))
    out_basis = normal_values(seeds[7], (QW, RANK), QW ** -0.5, 0.1875, ((0, 8),))
    query_mean = normal_values(seeds[8], (RANK, QW), 1.0, 6.0, ((0, 8), (1, 4)), jnp.float32)
    query_square = jnp.clip(jnp.exp(math.log(2.0) - 1.3862944 * jax.random.uniform(seeds[9], (RANK, QW), jnp.float32) ** block_scale(seeds[9], (RANK, QW), ((0, 8), (1, 4)), -0.2, 0.2)), 0.5, 2.0)
    out_mean = normal_values(seeds[10], (RANK, D), 1.0, 6.0, ((0, 8), (1, 4)), jnp.float32)
    out_square = jnp.clip(jnp.exp(math.log(2.0) - 1.3862944 * jax.random.uniform(seeds[11], (RANK, D), jnp.float32) ** block_scale(seeds[11], (RANK, D), ((0, 8), (1, 4)), -0.2, 0.2)), 0.5, 2.0)
    return dict(normed_inputs=normed_inputs, query_cotangent=query_cotangent, head_outputs=head_outputs, output_cotangent=output_cotangent, query_weight=query_weight, out_weight=out_weight, query_basis=query_basis, out_basis=out_basis, query_mean=query_mean, query_square=query_square, out_mean=out_mean, out_square=out_square)


def update_matrix(grad, basis, mean, square, weight):
    wide_basis = basis.astype(jnp.float32)
    reduced = jnp.dot(wide_basis.T, grad, precision=lax.Precision.HIGHEST)
    mean_new = 0.8 * mean + 0.2 * reduced
    square_new = 0.9 * square + 0.1 * reduced * reduced
    direction = mean_new / (jnp.sqrt(square_new) + 1e-08)
    full = jnp.dot(wide_basis, direction, precision=lax.Precision.HIGHEST)
    step = full * lax.rsqrt(lax.optimization_barrier(jnp.mean(full * full, axis=0)) + 0.05)
    weight_new = weight - 0.01 * step
    return (mean_new, square_new, step, weight_new, weight_new.astype(jnp.bfloat16))

def reference(normed_inputs, query_cotangent, head_outputs, output_cotangent, query_weight, out_weight, query_basis, out_basis, query_mean, query_square, out_mean, out_square):
    blocks = TOKENS // TOK_DEV
    inputs_blocks = normed_inputs.reshape(blocks, TOK_DEV, D)
    query_blocks = query_cotangent.reshape(blocks, TOK_DEV, QW)
    heads_blocks = head_outputs.reshape(blocks, TOK_DEV, QW)
    output_blocks = output_cotangent.reshape(blocks, TOK_DEV, D)

    def accumulate(totals, pieces):
        inputs_part, query_part, heads_part, output_part = pieces
        query_total = totals[0] + jnp.dot(inputs_part.astype(jnp.float32).T, query_part.astype(jnp.float32), precision=lax.Precision.HIGHEST)
        out_total = totals[1] + jnp.dot(heads_part.astype(jnp.float32).T, output_part.astype(jnp.float32), precision=lax.Precision.HIGHEST)
        return ((query_total, out_total), None)
    start_totals = (jnp.zeros((D, QW), jnp.float32), jnp.zeros((QW, D), jnp.float32))
    totals, unused = lax.scan(accumulate, start_totals, (inputs_blocks, query_blocks, heads_blocks, output_blocks))
    token_scale = TOKENS ** (-0.5)
    query_grad = totals[0] * token_scale
    out_grad = totals[1] * token_scale
    query_results = update_matrix(query_grad, query_basis, query_mean, query_square, query_weight)
    out_results = update_matrix(out_grad, out_basis, out_mean, out_square, out_weight)
    return (query_results[0], query_results[1], query_results[2], query_results[3], query_results[4], out_results[0], out_results[1], out_results[2], out_results[3], out_results[4])
```

```python
import functools

import jax
import jax.numpy as jnp
from jax import lax
from jax.experimental import pallas as pl
from jax.experimental.pallas import tpu as pltpu
from jax.sharding import PartitionSpec as P

MESH = pl.DeviceIdType.MESH
F32 = jnp.float32
BF16 = jnp.bfloat16


def plane(fs_count):
    inner = 1
    while 2 * (2 * inner) ** 2 <= fs_count:
        inner *= 2
    return fs_count // inner, inner


def greet(peers):
    barrier = pltpu.get_barrier_semaphore()
    for peer in peers:
        pl.semaphore_signal(barrier, inc=1, device_id=peer, device_id_type=MESH)
    pl.semaphore_wait(barrier, len(peers))


def remote(src, dst, send, recv, peer):
    return pltpu.make_async_remote_copy(
        src_ref=src, dst_ref=dst, send_sem=send, recv_sem=recv, device_id=peer, device_id_type=MESH
    )


def gather_basis(Z, X, qb, ob, qall, oall, zs, zr, xs, xr, ps, pr):
    f, t = lax.axis_index("fs"), lax.axis_index("tp")
    z, x, c = f // X, lax.rem(f, X), lax.rem(t, 2)
    partner = (f, t + 1 - 2 * c)

    def zpeer(dz):
        return (lax.rem(z + dz, Z) * X + x, t)

    def xpeer(dx):
        return (z * X + lax.rem(x + dx, X), t)

    def source(dz, dx):
        return lax.rem(z + Z - dz, Z) * X + lax.rem(x + X - dx, X)

    greet([zpeer(d) for d in range(1, Z)] + [xpeer(d) for d in range(1, X)] + [partner])
    pairs = ((qb, qall), (ob, oall))
    sent = []

    def half(ref, rows, block, core):
        n = rows // 2
        return ref.at[pl.ds(pl.multiple_of(block * rows + core * n, n), n), :]

    def send(i, dz, dx, send_sem, recv_sem, peer):
        own, full = pairs[i]
        rows = own.shape[0]
        dst = half(full, rows, source(dz, dx), c)
        src = half(own, rows, 0, c) if dz == 0 and dx == 0 else dst
        copy = remote(src, dst, send_sem, recv_sem, peer)
        copy.start()
        sent.append(copy)

    def arrived(i, dz, dx, core, send_sem, recv_sem):
        own, full = pairs[i]
        ref = half(full, own.shape[0], source(dz, dx), core)
        remote(ref, ref, send_sem, recv_sem, partner).wait_recv()

    for dz in range(1, Z):
        for i in range(2):
            send(i, dz=0, dx=0, send_sem=zs.at[i, dz], recv_sem=zr.at[i, dz], peer=zpeer(dz))
    for dz in range(Z):
        for i in range(2):
            if dz:
                arrived(i, dz, 0, c, zs.at[i, dz], zr.at[i, dz])
            for dx in range(1, X):
                send(i, dz, 0, xs.at[i, dz, dx], xr.at[i, dz, dx], xpeer(dx))
            if dz:
                send(i, dz, 0, ps.at[i, dz, 0], pr.at[i, dz, 0], partner)
        if dz == 0:
            for own, full in pairs:
                rows = own.shape[0]
                full[pl.ds(pl.multiple_of(f * rows, rows), rows), :] = own[...]
    for dz in range(Z):
        for dx in range(1, X):
            for i in range(2):
                arrived(i, dz, dx, c, xs.at[i, dz, dx], xr.at[i, dz, dx])
                send(i, dz, dx, ps.at[i, dz, dx], pr.at[i, dz, dx], partner)
    for dz in range(Z):
        for dx in range(X):
            if dz or dx:
                for i in range(2):
                    arrived(i, dz, dx, 1 - c, ps.at[i, dz, dx], pr.at[i, dz, dx])
    for copy in sent:
        copy.wait_send()


def update(
    Z, X, Y, scale,
    parts_q, parts_o, wq, wo, mean_q, square_q, mean_o, square_o,
    dq, do, mq, sq, mo, so, wq_all, wo_all,
    r1q, r1o, s1q, s1o, r2q, r2o, s2q, s2o, r3q, r3o, s3q, s3o, r4q, r4o,
    s1s, s1r, s2s, s2r, s3s, s3r, s4s, s4r, gzs, gzr, gxs, gxr,
):
    f, t = lax.axis_index("fs"), lax.axis_index("tp")
    z, x, c, y = f // X, lax.rem(f, X), lax.rem(t, 2), t // 2
    partner = (f, t + 1 - 2 * c)
    rows = mean_q.shape[0]
    chunk = rows * X

    def zpeer(dz):
        return (lax.rem(z + dz, Z) * X + x, t)

    def xpeer(dx):
        return (z * X + lax.rem(x + dx, X), t)

    def ypeer(dy):
        return (f, lax.rem(y + dy, Y) * 2 + c)

    greet(
        [zpeer(d) for d in range(1, Z)]
        + [xpeer(d) for d in range(1, X)]
        + [ypeer(d) for d in range(1, Y)]
        + [partner]
    )
    sent = []

    def start(src, dst, send_sem, recv_sem, peer):
        copy = remote(src, dst, send_sem, recv_sem, peer)
        copy.start()
        sent.append(copy)

    def landed(dst, send_sem, recv_sem):
        remote(dst, dst, send_sem, recv_sem, partner).wait_recv()

    sides = (
        (parts_q, r1q, s1q, r2q, s2q, r3q, s3q, r4q),
        (parts_o, r1o, s1o, r2o, s2o, r3o, s3o, r4o),
    )
    gathers = (dq, do, wq_all, wo_all)
    heights = (rows, rows, wq.shape[0], wo.shape[0])

    def block(j, dz, dx):
        h = heights[j]
        b = lax.rem(z + Z - dz, Z) * X + lax.rem(x + X - dx, X)
        return gathers[j].at[pl.ds(pl.multiple_of(b * h, h), h), :]

    def spread(j, src):
        for dz in range(1, Z):
            start(src, block(j, 0, 0), gzs.at[j, dz], gzr.at[j, dz], zpeer(dz))
        for dx in range(1, X):
            start(src, block(j, 0, 0), gxs.at[j, 0, dx], gxr.at[j, 0, dx], xpeer(dx))

    def forward(j, dz):
        landed(block(j, dz, 0), gzs.at[j, dz], gzr.at[j, dz])
        for dx in range(1, X):
            start(block(j, dz, 0), block(j, dz, 0), gxs.at[j, dz, dx], gxr.at[j, dz, dx], xpeer(dx))

    def finish(j):
        for dz in range(Z):
            for dx in range(1, X):
                landed(block(j, dz, dx), gxs.at[j, dz, dx], gxr.at[j, dz, dx])

    order = [*range(1, Z), 0]

    def span(k):
        return pl.ds(pl.multiple_of(lax.rem(z + k, Z) * chunk, chunk), chunk)

    def columns(i, core, dy):
        width = sides[i][1].shape[-1]
        start_at = (lax.rem(y + dy, Y) * 2 + core) * width
        return pl.ds(pl.multiple_of(start_at, width), width)

    ys = [*range(1, Y), 0]
    for k in order:
        for dy in ys:
            for i in range(2):
                parts, r1 = sides[i][:2]
                start(
                    parts.at[span(k), columns(i, 1 - c, dy)], r1.at[dy, k],
                    s1s.at[i, dy, k], s1r.at[i, dy, k], partner,
                )
    for j, w in ((2, wq), (3, wo)):
        spread(j, w)
        h = heights[j]
        gathers[j][pl.ds(pl.multiple_of(f * h, h), h), :] = w[...]
    for k in order:
        for dy in ys:
            for i in range(2):
                parts, r1, s1, r2 = sides[i][:4]
                landed(r1.at[dy, k], s1s.at[i, dy, k], s1r.at[i, dy, k])
                s1[dy, k] = (parts[span(k), columns(i, c, dy)].astype(F32) + r1[dy, k].astype(F32)).astype(BF16)
                if dy:
                    start(s1.at[dy, k], r2.at[dy, k], s2s.at[i, dy, k], s2r.at[i, dy, k], ypeer(dy))

    def add_x(k):
        for i in range(2):
            s2, r3, s3, r4 = sides[i][4:]
            own = pl.ds(pl.multiple_of(x * rows, rows), rows)
            total = s2[k, own, :].astype(F32)
            for dx in range(1, X):
                landed(r3.at[dx, k], s3s.at[i, dx, k], s3r.at[i, dx, k])
                total += r3[dx, k].astype(F32)
            s3[k] = total.astype(BF16)
            if k:
                start(s3.at[k], r4.at[k], s4s.at[i, k], s4r.at[i, k], zpeer(k))

    for at, k in enumerate(order):
        for i in range(2):
            _, _, s1, r2, s2, r3 = sides[i][:6]
            total = s1[0, k].astype(F32)
            for dy in range(1, Y):
                landed(r2.at[dy, k], s2s.at[i, dy, k], s2r.at[i, dy, k])
                total += r2[dy, k].astype(F32)
            s2[k] = total.astype(BF16)
            for dx in range(1, X):
                there = pl.ds(pl.multiple_of(lax.rem(x + dx, X) * rows, rows), rows)
                start(s2.at[k, there, :], r3.at[dx, k], s3s.at[i, dx, k], s3r.at[i, dx, k], xpeer(dx))
        if at:
            add_x(order[at - 1])
    add_x(order[-1])
    for i, (mean, square, mean_new, square_new) in enumerate(
        ((mean_q, square_q, mq, sq), (mean_o, square_o, mo, so))
    ):
        s3, r4 = sides[i][6:]
        total = s3[0].astype(F32)
        for k in range(1, Z):
            landed(r4.at[k], s4s.at[i, k], s4r.at[i, k])
            total += r4[k].astype(F32)
        reduced = total * scale
        first = 0.8 * mean[...] + 0.2 * reduced
        second = 0.9 * square[...] + 0.1 * reduced * reduced
        mean_new[...] = first
        square_new[...] = second
        gathers[i][pl.ds(pl.multiple_of(f * rows, rows), rows), :] = (
            first / (jnp.sqrt(second) + 1e-08)
        ).astype(BF16)
        spread(i, block(i, 0, 0))
    for dz in range(1, Z):
        for j in (2, 3):
            forward(j, dz)
    for dz in range(1, Z):
        for j in (0, 1):
            forward(j, dz)
    for j in range(4):
        finish(j)
    for copy in sent:
        copy.wait_send()


def vmem(n):
    return [pl.BlockSpec(memory_space=pltpu.VMEM)] * n


def dma(*shape):
    return pltpu.SemaphoreType.DMA(shape)


def shards(
    normed_inputs, query_cotangent, head_outputs, output_cotangent, query_weight, out_weight,
    query_basis, out_basis, query_mean, query_square, out_mean, out_square,
):
    fs, tp = lax.axis_size("fs"), lax.axis_size("tp")
    Z, X = plane(fs)
    Y = tp // 2
    scale = (normed_inputs.shape[0] * fs * tp) ** (-0.5)
    model_rows, query_width = normed_inputs.shape[1], query_cotangent.shape[1]
    qc, oc = query_weight.shape[1], out_weight.shape[1]
    rows, rank = query_mean.shape[0], query_basis.shape[1]
    shape = jax.ShapeDtypeStruct
    query_all, out_all = pl.pallas_call(
        functools.partial(gather_basis, Z, X),
        out_shape=(shape((model_rows, rank), BF16), shape((query_width, rank), BF16)),
        in_specs=vmem(2),
        out_specs=vmem(2),
        scratch_shapes=[dma(2, Z), dma(2, Z), dma(2, Z, X), dma(2, Z, X), dma(2, Z, X), dma(2, Z, X)],
        compiler_params=pltpu.CompilerParams(collective_id=0, has_side_effects=True),
    )(query_basis, out_basis)
    contract = (((0,), (0,)), ((), ()))
    query_left = jnp.dot(normed_inputs, query_all, preferred_element_type=F32).astype(BF16)
    out_left = jnp.dot(head_outputs, out_all, preferred_element_type=F32).astype(BF16)
    parts_q = lax.dot_general(query_left, query_cotangent, contract, preferred_element_type=F32).astype(BF16)
    parts_o = lax.dot_general(out_left, output_cotangent, contract, preferred_element_type=F32).astype(BF16)

    def pair(*lead):
        return [pltpu.VMEM((*lead, qc), BF16), pltpu.VMEM((*lead, oc), BF16)]

    chunk = X * rows
    scratch = (
        pair(Y, Z, chunk) + pair(Y, Z, chunk) + pair(Y, Z, chunk) + pair(Z, chunk)
        + pair(X, Z, rows) + pair(Z, rows) + pair(Z, rows)
        + [dma(2, Y, Z)] * 4 + [dma(2, X, Z)] * 2 + [dma(2, Z)] * 2
        + [dma(4, Z)] * 2 + [dma(4, Z, X)] * 2
    )
    dq, do, mq, sq, mo, so, wq_all, wo_all = pl.pallas_call(
        functools.partial(update, Z, X, Y, scale),
        out_shape=(
            shape((rank, qc), BF16), shape((rank, oc), BF16),
            shape((rows, qc), F32), shape((rows, qc), F32),
            shape((rows, oc), F32), shape((rows, oc), F32),
            shape((model_rows, qc), BF16), shape((query_width, oc), BF16),
        ),
        in_specs=vmem(8),
        out_specs=vmem(8),
        scratch_shapes=scratch,
        compiler_params=pltpu.CompilerParams(collective_id=1, has_side_effects=True),
    )(
        parts_q, parts_o, query_weight.astype(BF16), out_weight.astype(BF16),
        query_mean, query_square, out_mean, out_square,
    )
    at = lax.axis_index("fs")

    def apply(basis, direction, weight, weight_all):
        full = jnp.dot(basis, direction, preferred_element_type=F32)
        gain = lax.rsqrt(jnp.sum(full * full, axis=0) / full.shape[0] + 0.05)
        copy = (weight_all.astype(F32) - 0.01 * (full * gain)).astype(BF16)
        step = lax.dynamic_slice_in_dim(full, at * weight.shape[0], weight.shape[0], 0) * gain
        return step, weight - 0.01 * step, copy

    query_out = apply(query_all, dq, query_weight, wq_all)
    out_out = apply(out_all, do, out_weight, wo_all)
    return (mq, sq, *query_out, mo, so, *out_out)


def solution(mesh):
    token = P(("fs", "tp"), None)
    both, row, column = P("fs", "tp"), P("fs", None), P(None, "tp")
    return jax.shard_map(
        shards,
        mesh=mesh,
        in_specs=(token,) * 4 + (both, both, row, row) + (both,) * 4,
        out_specs=(both, both, both, both, column) * 2,
        check_vma=False,
    )
```

```python
import functools

import jax
import jax.numpy as jnp
from jax import lax
from jax.experimental import pallas as pl
from jax.experimental.pallas import tpu as pltpu
from jax.sharding import PartitionSpec as P

MESH = pl.DeviceIdType.MESH
F32 = jnp.float32
BF16 = jnp.bfloat16


def plane(fs_count):
    inner = 1
    while 2 * (2 * inner) ** 2 <= fs_count:
        inner *= 2
    return fs_count // inner, inner


def greet(peers):
    barrier = pltpu.get_barrier_semaphore()
    for peer in peers:
        pl.semaphore_signal(barrier, inc=1, device_id=peer, device_id_type=MESH)
    pl.semaphore_wait(barrier, len(peers))


def remote(src, dst, send, recv, peer):
    return pltpu.make_async_remote_copy(
        src_ref=src, dst_ref=dst, send_sem=send, recv_sem=recv, device_id=peer, device_id_type=MESH
    )


def gather_basis(Z, X, qb, ob, qall, oall, zs, zr, xs, xr, ps, pr):
    f, t = lax.axis_index("fs"), lax.axis_index("tp")
    z, x, c = f // X, lax.rem(f, X), lax.rem(t, 2)
    partner = (f, t + 1 - 2 * c)

    def zpeer(dz):
        return (lax.rem(z + dz, Z) * X + x, t)

    def xpeer(dx):
        return (z * X + lax.rem(x + dx, X), t)

    def source(dz, dx):
        return lax.rem(z + Z - dz, Z) * X + lax.rem(x + X - dx, X)

    greet([zpeer(d) for d in range(1, Z)] + [xpeer(d) for d in range(1, X)] + [partner])
    pairs = ((qb, qall), (ob, oall))
    sent = []

    def half(ref, rows, block, core):
        n = rows // 2
        return ref.at[pl.ds(pl.multiple_of(block * rows + core * n, n), n), :]

    def send(i, dz, dx, send_sem, recv_sem, peer):
        own, full = pairs[i]
        rows = own.shape[0]
        dst = half(full, rows, source(dz, dx), c)
        src = half(own, rows, 0, c) if dz == 0 and dx == 0 else dst
        copy = remote(src, dst, send_sem, recv_sem, peer)
        copy.start()
        sent.append(copy)

    def arrived(i, dz, dx, core, send_sem, recv_sem):
        own, full = pairs[i]
        ref = half(full, own.shape[0], source(dz, dx), core)
        remote(ref, ref, send_sem, recv_sem, partner).wait_recv()

    for dz in range(1, Z):
        for i in range(2):
            send(i, dz=0, dx=0, send_sem=zs.at[i, dz], recv_sem=zr.at[i, dz], peer=zpeer(dz))
    for dz in range(Z):
        for i in range(2):
            if dz:
                arrived(i, dz, 0, c, zs.at[i, dz], zr.at[i, dz])
            for dx in range(1, X):
                send(i, dz, 0, xs.at[i, dz, dx], xr.at[i, dz, dx], xpeer(dx))
            if dz:
                send(i, dz, 0, ps.at[i, dz, 0], pr.at[i, dz, 0], partner)
        if dz == 0:
            for own, full in pairs:
                rows = own.shape[0]
                full[pl.ds(pl.multiple_of(f * rows, rows), rows), :] = own[...]
    for dz in range(Z):
        for dx in range(1, X):
            for i in range(2):
                arrived(i, dz, dx, c, xs.at[i, dz, dx], xr.at[i, dz, dx])
                send(i, dz, dx, ps.at[i, dz, dx], pr.at[i, dz, dx], partner)
    for dz in range(Z):
        for dx in range(X):
            if dz or dx:
                for i in range(2):
                    arrived(i, dz, dx, 1 - c, ps.at[i, dz, dx], pr.at[i, dz, dx])
    for copy in sent:
        copy.wait_send()


def update(
    Z, X, Y, scale,
    parts_q, parts_o, wq, wo, mean_q, square_q, mean_o, square_o,
    dq, do, mq, sq, mo, so, wq_all, wo_all,
    r1q, r1o, s1q, s1o, r2q, r2o, s2q, s2o, r3q, r3o, s3q, s3o, r4q, r4o,
    s1s, s1r, s2s, s2r, s3s, s3r, s4s, s4r, gzs, gzr, gxs, gxr,
):
    f, t = lax.axis_index("fs"), lax.axis_index("tp")
    z, x, c, y = f // X, lax.rem(f, X), lax.rem(t, 2), t // 2
    partner = (f, t + 1 - 2 * c)
    rows = mean_q.shape[0]
    chunk = rows * X

    def zpeer(dz):
        return (lax.rem(z + dz, Z) * X + x, t)

    def xpeer(dx):
        return (z * X + lax.rem(x + dx, X), t)

    def ypeer(dy):
        return (f, lax.rem(y + dy, Y) * 2 + c)

    greet(
        [zpeer(d) for d in range(1, Z)]
        + [xpeer(d) for d in range(1, X)]
        + [ypeer(d) for d in range(1, Y)]
        + [partner]
    )
    sent = []

    def start(src, dst, send_sem, recv_sem, peer):
        copy = remote(src, dst, send_sem, recv_sem, peer)
        copy.start()
        sent.append(copy)

    def landed(dst, send_sem, recv_sem):
        remote(dst, dst, send_sem, recv_sem, partner).wait_recv()

    sides = (
        (parts_q, r1q, s1q, r2q, s2q, r3q, s3q, r4q),
        (parts_o, r1o, s1o, r2o, s2o, r3o, s3o, r4o),
    )
    gathers = (dq, do, wq_all, wo_all)
    heights = (rows, rows, wq.shape[0], wo.shape[0])

    def block(j, dz, dx):
        h = heights[j]
        b = lax.rem(z + Z - dz, Z) * X + lax.rem(x + X - dx, X)
        return gathers[j].at[pl.ds(pl.multiple_of(b * h, h), h), :]

    def spread(j, src):
        for dz in range(1, Z):
            start(src, block(j, 0, 0), gzs.at[j, dz], gzr.at[j, dz], zpeer(dz))
        for dx in range(1, X):
            start(src, block(j, 0, 0), gxs.at[j, 0, dx], gxr.at[j, 0, dx], xpeer(dx))

    def forward(j, dz):
        landed(block(j, dz, 0), gzs.at[j, dz], gzr.at[j, dz])
        for dx in range(1, X):
            start(block(j, dz, 0), block(j, dz, 0), gxs.at[j, dz, dx], gxr.at[j, dz, dx], xpeer(dx))

    def finish(j):
        for dz in range(Z):
            for dx in range(1, X):
                landed(block(j, dz, dx), gxs.at[j, dz, dx], gxr.at[j, dz, dx])

    order = [*range(1, Z), 0]

    def span(k):
        return pl.ds(pl.multiple_of(lax.rem(z + k, Z) * chunk, chunk), chunk)

    def columns(i, core, dy):
        width = sides[i][1].shape[-1]
        start_at = (lax.rem(y + dy, Y) * 2 + core) * width
        return pl.ds(pl.multiple_of(start_at, width), width)

    ys = [*range(1, Y), 0]
    for k in order:
        for dy in ys:
            for i in range(2):
                parts, r1 = sides[i][:2]
                start(
                    parts.at[span(k), columns(i, 1 - c, dy)], r1.at[dy, k],
                    s1s.at[i, dy, k], s1r.at[i, dy, k], partner,
                )
    for j, w in ((2, wq), (3, wo)):
        spread(j, w)
        h = heights[j]
        gathers[j][pl.ds(pl.multiple_of(f * h, h), h), :] = w[...]
    for k in order:
        for dy in ys:
            for i in range(2):
                parts, r1, s1, r2 = sides[i][:4]
                landed(r1.at[dy, k], s1s.at[i, dy, k], s1r.at[i, dy, k])
                s1[dy, k] = (parts[span(k), columns(i, c, dy)].astype(F32) + r1[dy, k].astype(F32)).astype(BF16)
                if dy:
                    start(s1.at[dy, k], r2.at[dy, k], s2s.at[i, dy, k], s2r.at[i, dy, k], ypeer(dy))

    def add_x(k):
        for i in range(2):
            s2, r3, s3, r4 = sides[i][4:]
            own = pl.ds(pl.multiple_of(x * rows, rows), rows)
            total = s2[k, own, :].astype(F32)
            for dx in range(1, X):
                landed(r3.at[dx, k], s3s.at[i, dx, k], s3r.at[i, dx, k])
                total += r3[dx, k].astype(F32)
            s3[k] = total.astype(BF16)
            if k:
                start(s3.at[k], r4.at[k], s4s.at[i, k], s4r.at[i, k], zpeer(k))

    for at, k in enumerate(order):
        for i in range(2):
            _, _, s1, r2, s2, r3 = sides[i][:6]
            total = s1[0, k].astype(F32)
            for dy in range(1, Y):
                landed(r2.at[dy, k], s2s.at[i, dy, k], s2r.at[i, dy, k])
                total += r2[dy, k].astype(F32)
            s2[k] = total.astype(BF16)
            for dx in range(1, X):
                there = pl.ds(pl.multiple_of(lax.rem(x + dx, X) * rows, rows), rows)
                start(s2.at[k, there, :], r3.at[dx, k], s3s.at[i, dx, k], s3r.at[i, dx, k], xpeer(dx))
        if at:
            add_x(order[at - 1])
        if at > 1:
            for j in (2, 3):
                forward(j, at - 1)
    add_x(order[-1])
    for j in (2, 3):
        forward(j, Z - 1)
    for i, (mean, square, mean_new, square_new) in enumerate(
        ((mean_q, square_q, mq, sq), (mean_o, square_o, mo, so))
    ):
        s3, r4 = sides[i][6:]
        total = s3[0].astype(F32)
        for k in range(1, Z):
            landed(r4.at[k], s4s.at[i, k], s4r.at[i, k])
            total += r4[k].astype(F32)
        reduced = total * scale
        first = 0.8 * mean[...] + 0.2 * reduced
        second = 0.9 * square[...] + 0.1 * reduced * reduced
        mean_new[...] = first
        square_new[...] = second
        gathers[i][pl.ds(pl.multiple_of(f * rows, rows), rows), :] = (
            first / (jnp.sqrt(second) + 1e-08)
        ).astype(BF16)
        spread(i, block(i, 0, 0))
    for dz in range(1, Z):
        for j in (0, 1):
            forward(j, dz)
    for j in range(4):
        finish(j)
    for copy in sent:
        copy.wait_send()


def vmem(n):
    return [pl.BlockSpec(memory_space=pltpu.VMEM)] * n


def dma(*shape):
    return pltpu.SemaphoreType.DMA(shape)


def shards(
    normed_inputs, query_cotangent, head_outputs, output_cotangent, query_weight, out_weight,
    query_basis, out_basis, query_mean, query_square, out_mean, out_square,
):
    fs, tp = lax.axis_size("fs"), lax.axis_size("tp")
    Z, X = plane(fs)
    Y = tp // 2
    scale = (normed_inputs.shape[0] * fs * tp) ** (-0.5)
    model_rows, query_width = normed_inputs.shape[1], query_cotangent.shape[1]
    qc, oc = query_weight.shape[1], out_weight.shape[1]
    rows, rank = query_mean.shape[0], query_basis.shape[1]
    shape = jax.ShapeDtypeStruct
    query_all, out_all = pl.pallas_call(
        functools.partial(gather_basis, Z, X),
        out_shape=(shape((model_rows, rank), BF16), shape((query_width, rank), BF16)),
        in_specs=vmem(2),
        out_specs=vmem(2),
        scratch_shapes=[dma(2, Z), dma(2, Z), dma(2, Z, X), dma(2, Z, X), dma(2, Z, X), dma(2, Z, X)],
        compiler_params=pltpu.CompilerParams(collective_id=0, has_side_effects=True),
    )(query_basis, out_basis)
    contract = (((0,), (0,)), ((), ()))
    query_left = jnp.dot(normed_inputs, query_all, preferred_element_type=F32).astype(BF16)
    out_left = jnp.dot(head_outputs, out_all, preferred_element_type=F32).astype(BF16)
    parts_q = lax.dot_general(query_left, query_cotangent, contract, preferred_element_type=F32).astype(BF16)
    parts_o = lax.dot_general(out_left, output_cotangent, contract, preferred_element_type=F32).astype(BF16)

    def pair(*lead):
        return [pltpu.VMEM((*lead, qc), BF16), pltpu.VMEM((*lead, oc), BF16)]

    chunk = X * rows
    scratch = (
        pair(Y, Z, chunk) + pair(Y, Z, chunk) + pair(Y, Z, chunk) + pair(Z, chunk)
        + pair(X, Z, rows) + pair(Z, rows) + pair(Z, rows)
        + [dma(2, Y, Z)] * 4 + [dma(2, X, Z)] * 2 + [dma(2, Z)] * 2
        + [dma(4, Z)] * 2 + [dma(4, Z, X)] * 2
    )
    dq, do, mq, sq, mo, so, wq_all, wo_all = pl.pallas_call(
        functools.partial(update, Z, X, Y, scale),
        out_shape=(
            shape((rank, qc), BF16), shape((rank, oc), BF16),
            shape((rows, qc), F32), shape((rows, qc), F32),
            shape((rows, oc), F32), shape((rows, oc), F32),
            shape((model_rows, qc), BF16), shape((query_width, oc), BF16),
        ),
        in_specs=vmem(8),
        out_specs=vmem(8),
        scratch_shapes=scratch,
        compiler_params=pltpu.CompilerParams(collective_id=1, has_side_effects=True),
    )(
        parts_q, parts_o, query_weight.astype(BF16), out_weight.astype(BF16),
        query_mean, query_square, out_mean, out_square,
    )
    at = lax.axis_index("fs")

    def apply(basis, direction, weight, weight_all):
        full = jnp.dot(basis, direction, preferred_element_type=F32)
        gain = lax.rsqrt(jnp.sum(full * full, axis=0) / full.shape[0] + 0.05)
        copy = (weight_all.astype(F32) - 0.01 * (full * gain)).astype(BF16)
        step = lax.dynamic_slice_in_dim(full, at * weight.shape[0], weight.shape[0], 0) * gain
        return step, weight - 0.01 * step, copy

    query_out = apply(query_all, dq, query_weight, wq_all)
    out_out = apply(out_all, do, out_weight, wo_all)
    return (mq, sq, *query_out, mo, so, *out_out)


def solution(mesh):
    token = P(("fs", "tp"), None)
    both, row, column = P("fs", "tp"), P("fs", None), P(None, "tp")
    return jax.shard_map(
        shards,
        mesh=mesh,
        in_specs=(token,) * 4 + (both, both, row, row) + (both,) * 4,
        out_specs=(both, both, both, both, column) * 2,
        check_vma=False,
    )
```
